1024 devices in a mesh: rep: 32 (over z), fs: 4 (over y), tp: 8 (over x, core).
Axes of the slice: x: 4, y: 4, z: 32, core: 2. Of those that a mesh axis runs over, the one named last changes fastest.
Arguments:
- inputs: bfloat16 [20480, 2048], P('rep', 'fs'), may hold values from -6 to 6
- gate_pre: bfloat16 [20480, 5632], P('rep', 'tp'), may hold values from -12 to 12
- up_pre: bfloat16 [20480, 5632], P('rep', 'tp'), may hold values from -6 to 6
- cotangent: bfloat16 [20480, 2048], P('rep'), may hold values from -6 to 6
- w_gate: bfloat16 [2048, 5632], P('fs', 'tp'), may hold values from -0.125 to 0.125
- w_up: bfloat16 [2048, 5632], P('fs', 'tp'), may hold values from -0.125 to 0.125
- w_down: bfloat16 [5632, 2048], P('tp', 'fs'), may hold values from -0.078125 to 0.078125
Outputs:
- grad_input: bfloat16 [20480, 2048], P('rep', 'fs')
- grad_gate: float32 [64, 32, 5632], P('fs', 'rep', 'tp')
- grad_up: float32 [64, 32, 5632], P('fs', 'rep', 'tp')
- grad_down: float32 [5632, 64, 32], P('tp', 'fs', 'rep')
- gate_norms: float32 [64, 32], P('fs', 'rep')
- up_norms: float32 [64, 32], P('fs', 'rep')
- down_norms: float32 [5632], P('tp')
The draws below stay inside these ranges and needn't reach their ends.
All inputs are finite; a program needn't handle non-finite values.
Results may differ from the reference program's by a relative error of at most 0.02.
Values may be sent and summed in bfloat16 or wider, within the bound.
A program may use at most 64 MiB of HBM per device.

```python
import jax
import jax.numpy as jnp
from jax import lax

D = 2048
FF = 5632
TOKENS = 20480
N_REP = 32
N_TP = 8


def raised(values, key, source, target, shards_of, factor):
    def block_of(position):
        return (jnp.arange(values.shape[position]) // (values.shape[position] // shards_of)).reshape((-1,) + (1,) * (values.ndim - 1 - position))

    first = jax.random.permutation(key, shards_of)[block_of(target)]
    far = (block_of(target) + shards_of // 2) % shards_of
    return jnp.where((block_of(source) == first) | (block_of(source) == far), factor * values, values)


def level_of(own_key, shape, pieces, smallest, high):
    def one(dim, blocks):
        heights = jax.random.uniform(jax.random.fold_in(jax.random.fold_in(own_key, 6), dim), (blocks,), jnp.float32, smallest / len(pieces), high / len(pieces))
        return jnp.repeat(jnp.exp(heights), shape[dim] // blocks).reshape((-1,) + (1,) * (len(shape) - dim - 1))

    level = one(*pieces[0])
    for cut in pieces[1:]:
        level = level * one(*cut)
    return level


def bell_draw(own_key, shape, scale, bound, shards=(), kind=jnp.bfloat16):
    loudness = level_of(own_key, shape, shards, -0.22, 0.18) if shards else 1.0
    drawn = jax.random.normal(own_key, shape, jnp.float32) * scale * loudness
    return jnp.minimum(jnp.maximum(drawn, -bound), bound).astype(kind)


def heavy_noise(key, extent, deviation, most, pieces, heavy, held_as=jnp.bfloat16):
    entries = deviation * jax.random.normal(key, extent, jnp.float32)
    if pieces:
        entries = entries * level_of(key, extent, pieces, -0.22, 0.18)
    return jnp.clip(raised(entries, jax.random.fold_in(key, 3), *heavy), -most, most).astype(held_as)


def setup_inputs(seed: int = 0) -> dict:
    streams_of = jax.random.split(jax.random.key(seed), 8)
    return {
        "inputs": bell_draw(streams_of[0], (TOKENS, D), 1.0, 6.0, ((0, 32), (1, 4))),
        "gate_pre": bell_draw(streams_of[1], (TOKENS, FF), 2.0, 12.0, ((0, 32), (1, 8))),
        "up_pre": bell_draw(streams_of[2], (TOKENS, FF), 1.0, 6.0, ((0, 32), (1, 8))),
        "cotangent": heavy_noise(streams_of[3], (TOKENS, D), 1.0, 6.0, ((0, 32),), (0, 1, 32, 2.75)),
        "w_gate": bell_draw(streams_of[4], (D, FF), D ** -0.5, 0.125, ((0, 4), (1, 8))),
        "w_up": bell_draw(streams_of[5], (D, FF), D ** -0.5, 0.125, ((0, 4), (1, 8))),
        "w_down": bell_draw(streams_of[6], (FF, D), FF ** -0.5, 0.078125, ((0, 8), (1, 4))),
    }


def reference(inputs, gate_pre, up_pre, cotangent, w_gate, w_up, w_down):
    single = jnp.float32
    hidden_grad = jnp.dot(cotangent, w_down.T, preferred_element_type=single)
    gate = gate_pre.astype(single)
    upper = up_pre.astype(single)
    sigma = jax.nn.sigmoid(gate)
    active = gate * sigma
    hidden = (active * upper).astype(jnp.bfloat16)
    d_up = (hidden_grad * active).astype(jnp.bfloat16)
    d_gate = (hidden_grad * upper * sigma * (1.0 + gate * (1.0 - sigma))).astype(jnp.bfloat16)
    factor = float(TOKENS) ** -0.5
    grad_gate = jnp.dot(inputs.T, d_gate, preferred_element_type=single) * factor
    grad_up = jnp.dot(inputs.T, d_up, preferred_element_type=single) * factor
    grad_down = jnp.dot(hidden.T, cotangent, preferred_element_type=single) * factor
    block = FF // N_TP
    total = jnp.zeros(inputs.shape, single)
    for index in range(N_TP):
        lower = index * block
        term = jnp.dot(d_gate[:, lower:lower + block], w_gate[:, lower:lower + block].T, preferred_element_type=single)
        term = term + jnp.dot(d_up[:, lower:lower + block], w_up[:, lower:lower + block].T, preferred_element_type=single)
        term = lax.optimization_barrier(term.astype(jnp.bfloat16)).astype(single)
        total = total + term
    grad_input = total.astype(jnp.bfloat16)
    gate_norms = jnp.sum(grad_gate * grad_gate, axis=1).reshape(D // N_REP, N_REP)
    up_norms = jnp.sum(grad_up * grad_up, axis=1).reshape(D // N_REP, N_REP)
    down_norms = jnp.sum(grad_down * grad_down, axis=1)
    return (grad_input, grad_gate.reshape(D // N_REP, N_REP, FF), grad_up.reshape(D // N_REP, N_REP, FF),
            grad_down.reshape(FF, D // N_REP, N_REP), gate_norms, up_norms, down_norms)
```

```python
import functools

import jax
import jax.numpy as jnp
from jax import lax
from jax.experimental import pallas as pl
from jax.experimental.pallas import tpu as pltpu
from jax.sharding import PartitionSpec as P

MESH = pl.DeviceIdType.MESH
SINGLE = jnp.float32
HALF = jnp.bfloat16
STRIDES = (1, 1, 1, 1, 1)


def dot_nt(a, b):
    return lax.dot_general(a, b, (((1,), (1,)), ((), ())), preferred_element_type=SINGLE)


def dot_tn(a, b):
    return lax.dot_general(a, b, (((0,), (0,)), ((), ())), preferred_element_type=SINGLE)


def chains_of(groups, stride):
    half = groups // 2
    found = []
    for way, far in ((1, half), (-1, groups - 1 - half)):
        for shift in range(stride):
            start = far - shift
            found.append((way, start, stride, -(-start // stride)))
    return found


def kernel(
    sizes,
    x_ref, g_ref, u_ref, cot_ref, wg_ref, wu_ref, wd_ref,
    gi_ref, gg_ref, gu_ref, gd_ref, gn_ref, un_ref, dn_ref,
    xv, gv, uv, cv, wcat, wq, relay_a, relay_b, hgb, cg, cu, hid, xp, cp, dall,
    down, quart, stage_d, stage_q, buf_d, buf_q, fin, term, parts, res,
    nvec, nrecv, dmine, dy, dgroup, dfar,
    load_sem, a2a_s, a2a_r, hg_s, hg_r, ds_sem, dr_sem, qs_sem, qr_sem,
    ti_s, ti_r, to_s, to_r, n_s, n_r, m_s, m_r, out_sem,
):
    nr, nf, nt = sizes
    tokens, width = xv.shape
    hunits = gv.shape[0]
    q = hunits // nf
    own = width // nr
    top = -(-q // 32) * 16
    low = q - top
    rows = tokens // nt
    factor = float(tokens * nr) ** -0.5
    z, y, t = (lax.axis_index(name) for name in ("rep", "fs", "tp"))
    right, left, across = (lax.rem(y + step, nf) for step in (1, nf - 1, nf // 2))
    order = (y, left, right, across)

    def rep(step):
        return lax.rem(z + step + nr, nr)

    def at(rz=None, ry=None, rt=None):
        return (z if rz is None else rz, y if ry is None else ry, t if rt is None else rt)

    def remote(src, dst, ssem, rsem, device):
        return pltpu.make_async_remote_copy(
            src_ref=src, dst_ref=dst, send_sem=ssem, recv_sem=rsem, device_id=device, device_id_type=MESH
        )

    def arrived(ref, rsem):
        remote(ref, ref, rsem, rsem, at(ry=right)).wait_recv()

    def mult(value, by):
        return pl.multiple_of(value * by, by)

    sent = []

    def send(*args):
        copy = remote(*args)
        copy.start()
        sent.append(copy)

    loads = {}

    def load(name, src, dst):
        copy = pltpu.make_async_copy(src, dst, load_sem.at[len(loads)])
        copy.start()
        loads[name] = copy

    load("g", g_ref, gv)
    load("u", u_ref, uv)
    load("c", cot_ref, cv)
    load("x", x_ref, xv)
    load("wq", wd_ref.at[pl.ds(mult(y, q), q)], wq.at[y])
    for j in range(nf):
        load(f"wg{j}", wg_ref.at[pl.ds(j * q, q)], wcat.at[j, pl.ds(0, q)])
        load(f"wu{j}", wu_ref.at[pl.ds(j * q, q)], wcat.at[j, pl.ds(q, q)])

    barrier = pltpu.get_barrier_semaphore()
    near = [at(rz=rep(way * step)) for step in (1, 2, 3) for way in (1, -1)]
    near += [at(ry=lax.rem(y + step, nf)) for step in range(1, nf)]
    near += [at(rt=lax.rem(t + step, nt)) for step in range(1, nt)]
    for device in near:
        pl.semaphore_signal(barrier, inc=1, device_id=device, device_id_type=MESH)
    pl.semaphore_wait(barrier, len(near))

    far_a = wd_ref.at[pl.ds(pl.multiple_of(across * q, 16), top)]
    far_b = wd_ref.at[pl.ds(pl.multiple_of(across * q + top, 16), low)]
    send(far_a, relay_a, a2a_s.at[0], a2a_r.at[0], at(ry=right))
    send(far_b, relay_b, a2a_s.at[1], a2a_r.at[1], at(ry=left))
    send(wd_ref.at[pl.ds(mult(right, q), q)], wq.at[y], a2a_s.at[2], a2a_r.at[2], at(ry=right))
    send(wd_ref.at[pl.ds(mult(left, q), q)], wq.at[y], a2a_s.at[3], a2a_r.at[3], at(ry=left))

    loads["g"].wait()
    loads["u"].wait()
    step_rows = 16

    def factors(index, carry):
        span = pl.ds(pl.multiple_of(index * step_rows, step_rows), step_rows)
        gate = gv[span, :].astype(SINGLE)
        upper = uv[span, :].astype(SINGLE)
        sigma = 1.0 / (1.0 + jnp.exp(-gate))
        active = gate * sigma
        cu[span, :] = active
        hid[span, :] = (active * upper).astype(HALF)
        cg[span, :] = upper * sigma * (1.0 + gate * (1.0 - sigma))
        return carry

    lax.fori_loop(0, hunits // step_rows, factors, 0)

    place = lax.broadcasted_iota(jnp.int32, (width, width), 0)
    column = lax.broadcasted_iota(jnp.int32, (width, width), 1)
    bits = own.bit_length() - 1
    origin = (place & (own - 1)) * nr + (place >> bits)
    pick = jnp.where(column == origin, 1.0, 0.0).astype(HALF)
    loads["c"].wait()
    cp[...] = dot_nt(pick, cv[:, pl.ds(mult(y, width), width)]).astype(HALF)
    down[...] = dot_nt(cp[...], hid[...]) * factor

    specs = [chains_of(nr, stride) for stride in STRIDES]

    def tables(s):
        if s == 0:
            return down, stage_d, buf_d, ds_sem, dr_sem
        i = s - 1
        return quart.at[i], stage_q.at[i], buf_q.at[i], qs_sem.at[i], qr_sem.at[i]

    clock = [0] * len(specs)

    def local(mine, owner):
        return mine[pl.ds(mult(owner, own), own), :]

    def tick(s):
        tau = clock[s]
        clock[s] += 1
        mine, stage, buf, ssem, rsem = tables(s)
        done = []
        for c, (way, far, stride, steps) in enumerate(specs[s]):
            if tau > steps:
                continue
            distance = far - stride * tau
            if tau == 0:
                src = stage.at[c]
                src[...] = local(mine, rep(way * distance)).astype(HALF)
            else:
                src = buf.at[c, tau - 1]
                arrived(src, rsem.at[c, tau - 1])
                if tau == steps:
                    continue
                total = src[...].astype(SINGLE) + local(mine, rep(way * distance))
                src[...] = total.astype(HALF)
            send(src, buf.at[c, tau], ssem.at[c, tau], rsem.at[c, tau], at(rz=rep(way * min(stride, distance))))

    def length(s):
        return max(steps for _, _, _, steps in specs[s])

    def total_of(s):
        mine, _, buf, _, _ = tables(s)
        total = local(mine, z)
        for c, (_, _, _, steps) in enumerate(specs[s]):
            total = total + buf[c, steps - 1].astype(SINGLE)
        return total

    tick(0)

    loads["x"].wait()
    xp[...] = dot_nt(pick, xv[...]).astype(HALF)

    arrived(relay_a, a2a_r.at[0])
    send(relay_a, wq.at[left, pl.ds(0, top)], a2a_s.at[4], a2a_r.at[4], at(ry=right))
    arrived(relay_b, a2a_r.at[1])
    send(relay_b, wq.at[right, pl.ds(top, low)], a2a_s.at[5], a2a_r.at[5], at(ry=left))
    tick(0)

    def piece(j):
        return dot_nt(wq[j], cv[:, pl.ds(mult(j, width), width)])

    loads["wq"].wait()
    arrived(wq.at[left], a2a_r.at[2])
    arrived(wq.at[right], a2a_r.at[3])
    part = piece(y) + piece(left) + piece(right)
    tick(0)
    arrived(wq.at[across, pl.ds(0, top)], a2a_r.at[4])
    arrived(wq.at[across, pl.ds(top, low)], a2a_r.at[5])
    hgb[y] = (part + piece(across)).astype(HALF)
    upper_rows, lower_rows = pl.ds(0, top), pl.ds(top, low)
    send(hgb.at[y, upper_rows], hgb.at[y, upper_rows], hg_s.at[0], hg_r.at[0], at(ry=right))
    send(hgb.at[y, lower_rows], hgb.at[y, lower_rows], hg_s.at[1], hg_r.at[1], at(ry=left))
    send(hgb.at[y, lower_rows], hgb.at[y, lower_rows], hg_s.at[2], hg_r.at[2], at(ry=right))
    send(hgb.at[y, upper_rows], hgb.at[y, upper_rows], hg_s.at[3], hg_r.at[3], at(ry=left))

    def quarter(i):
        j = order[i]
        span = pl.ds(mult(j, q), q)
        grad = hgb[j].astype(SINGLE)
        dall[i, 0:q, :] = (grad * cg[span, :]).astype(HALF)
        dall[i, q : 2 * q, :] = (grad * cu[span, :]).astype(HALF)
        quart[i] = dot_nt(xp[...], dall[i]) * factor
        tick(1 + i)

    quarter(0)
    tick(0)
    tick(1)
    arrived(hgb.at[left, upper_rows], hg_r.at[0])
    send(hgb.at[left, upper_rows], hgb.at[left, upper_rows], hg_s.at[4], hg_r.at[4], at(ry=right))
    arrived(hgb.at[right, lower_rows], hg_r.at[1])
    send(hgb.at[right, lower_rows], hgb.at[right, lower_rows], hg_s.at[5], hg_r.at[5], at(ry=left))
    tick(0)
    tick(1)
    arrived(hgb.at[left, lower_rows], hg_r.at[2])
    quarter(1)
    arrived(hgb.at[right, upper_rows], hg_r.at[3])
    quarter(2)
    tick(0)
    tick(1)
    arrived(hgb.at[across, upper_rows], hg_r.at[4])
    arrived(hgb.at[across, lower_rows], hg_r.at[5])
    quarter(3)

    for name in [f"w{kind}{j}" for kind in "gu" for j in range(nf)]:
        loads[name].wait()

    block = 128

    def terms(n):
        span = pl.ds(n * block, block)
        total = dot_tn(dall[0, :, span], wcat[order[0]])
        for i in range(1, nf):
            total = total + dot_tn(dall[i, :, span], wcat[order[i]])
        term[span, :] = total.astype(HALF)

    peers = [lax.rem(t + step, nt) for step in range(1, nt)]

    def terms_out():
        for n, peer in enumerate(peers):
            send(term.at[pl.ds(mult(peer, rows), rows)], parts.at[t], ti_s.at[n], ti_r.at[n], at(rt=peer))
        parts[t] = term[pl.ds(mult(t, rows), rows), :]

    def sources():
        return [lax.rem(t + nt - step, nt) for step in range(1, nt)]

    def terms_sum():
        for n, peer in enumerate(sources()):
            arrived(parts.at[peer], ti_r.at[n])
        total = parts[0].astype(SINGLE)
        for n in range(1, nt):
            total = total + parts[n].astype(SINGLE)
        res[...] = total.astype(HALF)
        for n, peer in enumerate(peers):
            send(res, gi_ref.at[t], to_s.at[n], to_r.at[n], at(rt=peer))
        pltpu.make_async_copy(res, gi_ref.at[t], out_sem).start()

    def terms_end():
        for n, peer in enumerate(sources()):
            arrived(gi_ref.at[peer], to_r.at[n])
        pltpu.make_async_copy(res, gi_ref.at[t], out_sem).wait()

    def exchange(slots, mine, count, base, device_of):
        slots[mine] = dmine[...]
        for step in range(1, count):
            n = base + step - 1
            send(dmine, slots.at[mine], m_s.at[n], m_r.at[n], device_of(lax.rem(mine + step, count)))

    def summed(slots, mine, count, base):
        for step in range(1, count):
            arrived(slots.at[lax.rem(mine + count - step, count)], m_r.at[base + step - 1])
        total = slots[0]
        for n in range(1, count):
            total = total + slots[n]
        return total

    group = 4
    inner, outer = lax.rem(z, group), z // group
    across_y = (dy, y, nf, 0)
    across_in = (dgroup, inner, group, nf - 1)
    across_out = (dfar, outer, nr // group, nf + group - 2)
    dscr = (dmine,)

    def down_first():
        total = total_of(0)
        gd_ref[...] = total
        dmine[...] = jnp.sum(total * total, axis=0, keepdims=True)
        exchange(*across_y, lambda p: at(ry=p))

    def down_second():
        nvalue = summed(*across_y)
        dgroup[inner] = nvalue
        for step in range(1, group):
            n = nf - 1 + step - 1
            peer = lax.rem(inner + step, group)
            send(dgroup.at[inner], dgroup.at[inner], m_s.at[n], m_r.at[n], at(rz=outer * group + peer))

    def down_third():
        dfar[outer] = summed(*across_in)
        count = nr // group
        for step in range(1, count):
            n = nf + group - 2 + step - 1
            peer = lax.rem(outer + step, count)
            send(dfar.at[outer], dfar.at[outer], m_s.at[n], m_r.at[n], at(rz=peer * group + inner))

    def down_last():
        dn_ref[...] = summed(*across_out)

    down_stage = [down_first, down_second, down_third]

    n_tick = 0
    while clock[4] <= length(4):
        n_tick += 1
        for s in (4, 3, 2, 1, 0):
            if clock[s] <= length(s):
                tick(s)
        if 1 <= n_tick <= tokens // block:
            terms(n_tick - 1)
            if n_tick == tokens // block:
                terms_out()
        if n_tick == tokens // block + 5:
            terms_sum()
        if clock[0] > length(0) and down_stage:
            down_stage.pop(0)()
    while down_stage:
        down_stage.pop(0)()

    for i in range(nf):
        fin[order[i]] = total_of(1 + i)
    gate_total = jnp.zeros((own, 1), SINGLE)
    up_total = jnp.zeros((own, 1), SINGLE)
    for j in range(nf):
        gate_part, up_part = fin[j, :, 0:q], fin[j, :, q : 2 * q]
        gg_ref[:, j * q : (j + 1) * q] = gate_part
        gu_ref[:, j * q : (j + 1) * q] = up_part
        gate_total = gate_total + jnp.sum(gate_part * gate_part, axis=1, keepdims=True)
        up_total = up_total + jnp.sum(up_part * up_part, axis=1, keepdims=True)
    lane = lax.broadcasted_iota(jnp.int32, (own, 128), 1)
    nvec[...] = jnp.where(lane < 64, gate_total, up_total)
    nrecv[t] = nvec[...]
    for n, peer in enumerate(peers):
        send(nvec, nrecv.at[t], n_s.at[n], n_r.at[n], at(rt=peer))
    terms_end()
    for n, peer in enumerate(sources()):
        arrived(nrecv.at[peer], n_r.at[n])
    norms = nrecv[0]
    for n in range(1, nt):
        norms = norms + nrecv[n]
    turned = norms.T
    gn_ref[...] = turned[0:1, :]
    un_ref[...] = turned[64:65, :]
    down_last()
    for copy in sent:
        copy.wait_send()


def on_device(inputs, gate_pre, up_pre, cotangent, w_gate, w_up, w_down):
    nr, nf, nt = (lax.axis_size(name) for name in ("rep", "fs", "tp"))
    tokens, width = inputs.shape
    hunits = w_gate.shape[1]
    q, own, rows = hunits // nf, width // nr, tokens // nt
    top = -(-q // 32) * 16
    features = cotangent.shape[1]
    chain_count = [2 * stride for stride in STRIDES]
    many = max(chain_count[1:])
    long_d = -(-(nr // 2) // STRIDES[0])
    long_q = max(-(-(nr // 2) // stride) for stride in STRIDES[1:])
    vmem, dma = pltpu.VMEM, pltpu.SemaphoreType.DMA
    any_space = pl.BlockSpec(memory_space=pl.ANY)
    in_vmem = pl.BlockSpec(memory_space=pltpu.VMEM)
    shape = jax.ShapeDtypeStruct
    small = (nf - 1) + 3 + (nr // 4 - 1)
    gi, gg, gu, gd, gn, un, dn = pl.pallas_call(
        functools.partial(kernel, (nr, nf, nt)),
        out_shape=(
            shape((nt, rows, width), HALF),
            shape((own, hunits), SINGLE),
            shape((own, hunits), SINGLE),
            shape((own, hunits), SINGLE),
            shape((1, own), SINGLE),
            shape((1, own), SINGLE),
            shape((1, hunits), SINGLE),
        ),
        in_specs=[any_space] * 7,
        out_specs=(any_space,) + (in_vmem,) * 6,
        scratch_shapes=[
            vmem((tokens, width), HALF),
            vmem((hunits, tokens), HALF),
            vmem((hunits, tokens), HALF),
            vmem((tokens, features), HALF),
            vmem((nf, 2 * q, width), HALF),
            vmem((nf, q, width), HALF),
            vmem((top, width), HALF),
            vmem((q - top, width), HALF),
            vmem((nf, q, tokens), HALF),
            vmem((hunits, tokens), SINGLE),
            vmem((hunits, tokens), SINGLE),
            vmem((hunits, tokens), HALF),
            vmem((width, tokens), HALF),
            vmem((width, tokens), HALF),
            vmem((nf, 2 * q, tokens), HALF),
            vmem((width, hunits), SINGLE),
            vmem((nf, width, 2 * q), SINGLE),
            vmem((chain_count[0], own, hunits), HALF),
            vmem((nf, many, own, 2 * q), HALF),
            vmem((chain_count[0], long_d, own, hunits), HALF),
            vmem((nf, many, long_q, own, 2 * q), HALF),
            vmem((nf, own, 2 * q), SINGLE),
            vmem((tokens, width), HALF),
            vmem((nt, rows, width), HALF),
            vmem((rows, width), HALF),
            vmem((own, 128), SINGLE),
            vmem((nt, own, 128), SINGLE),
            vmem((1, hunits), SINGLE),
            vmem((nf, 1, hunits), SINGLE),
            vmem((4, 1, hunits), SINGLE),
            vmem((nr // 4, 1, hunits), SINGLE),
            dma((5 + 2 * nf,)),
            dma((6,)),
            dma((6,)),
            dma((6,)),
            dma((6,)),
            dma((chain_count[0], long_d)),
            dma((chain_count[0], long_d)),
            dma((nf, many, long_q)),
            dma((nf, many, long_q)),
            dma((nt - 1,)),
            dma((nt - 1,)),
            dma((nt - 1,)),
            dma((nt - 1,)),
            dma((nt - 1,)),
            dma((nt - 1,)),
            dma((small,)),
            dma((small,)),
            dma(()),
        ],
        compiler_params=pltpu.CompilerParams(
            collective_id=0, has_side_effects=True, vmem_limit_bytes=56 * 2**20
        ),
    )(inputs, gate_pre.T, up_pre.T, cotangent, w_gate.T, w_up.T, w_down)
    return (
        gi.reshape(tokens, width),
        gg.reshape(own, 1, hunits),
        gu.reshape(own, 1, hunits),
        gd.T.reshape(hunits, own, 1),
        gn.reshape(own, 1),
        un.reshape(own, 1),
        dn.reshape(hunits),
    )


def solution(mesh):
    placed = (
        P("rep", "fs"),
        P("rep", "tp"),
        P("rep", "tp"),
        P("rep", None),
        P("fs", "tp"),
        P("fs", "tp"),
        P("tp", "fs"),
    )
    return jax.shard_map(
        on_device,
        mesh=mesh,
        in_specs=placed,
        out_specs=(
            P("rep", "fs"),
            P("fs", "rep", "tp"),
            P("fs", "rep", "tp"),
            P("tp", "fs", "rep"),
            P("fs", "rep"),
            P("fs", "rep"),
            P("tp"),
        ),
        check_vma=False,
    )
```

```python
import functools

import jax
import jax.numpy as jnp
from jax import lax
from jax.experimental import pallas as pl
from jax.experimental.pallas import tpu as pltpu
from jax.sharding import PartitionSpec as P

MESH = pl.DeviceIdType.MESH
SINGLE = jnp.float32
HALF = jnp.bfloat16
STRIDES = (2, 2, 2, 2, 2)
PER_TICK = 2
WAITS = 5
ROUND = (1, 0, 2, 3, 4)


def dot_nt(a, b):
    return lax.dot_general(a, b, (((1,), (1,)), ((), ())), preferred_element_type=SINGLE)


def dot_tn(a, b):
    return lax.dot_general(a, b, (((0,), (0,)), ((), ())), preferred_element_type=SINGLE)


def chains_of(groups, stride):
    half = groups // 2
    found = []
    for way, far in ((1, half), (-1, groups - 1 - half)):
        links = far // stride
        found.append((way, far, links, 0 if links * stride == far else 1))
    return found


def side_count(groups, stride):
    return (groups // 2 - 1) // stride + 1


def kernel(
    sizes,
    x_ref, g_ref, u_ref, cot_ref, wg_ref, wu_ref, wd_ref,
    gi_ref, gg_ref, gu_ref, gd_ref, gn_ref, un_ref, dn_ref,
    xv, gv, uv, cv, wcat, wq, relay_a, relay_b, hgb, cg, cu, hid, xp, cp, dall,
    fin, term, parts, res,
    nvec, nrecv, dmine, dy, dgroup, dfar,
    load_sem, a2a_s, a2a_r, hg_s, hg_r,
    ti_s, ti_r, to_s, to_r, n_s, n_r, m_s, m_r, out_sem, *chain_refs,
):
    nr, nf, nt = sizes
    tokens, width = xv.shape
    hunits = gv.shape[0]
    q = hunits // nf
    own = width // nr
    top = -(-q // 32) * 16
    low = q - top
    rows = tokens // nt
    factor = float(tokens * nr) ** -0.5
    z, y, t = (lax.axis_index(name) for name in ("rep", "fs", "tp"))
    right, left, across = (lax.rem(y + step, nf) for step in (1, nf - 1, nf // 2))
    order = (y, left, right, across)

    def rep(step):
        return lax.rem(z + step + nr, nr)

    def at(rz=None, ry=None, rt=None):
        return (z if rz is None else rz, y if ry is None else ry, t if rt is None else rt)

    def remote(src, dst, ssem, rsem, device):
        return pltpu.make_async_remote_copy(
            src_ref=src, dst_ref=dst, send_sem=ssem, recv_sem=rsem, device_id=device, device_id_type=MESH
        )

    def arrived(ref, rsem):
        remote(ref, ref, rsem, rsem, at(ry=right)).wait_recv()

    def mult(value, by):
        return pl.multiple_of(value * by, by)

    sent = []

    def send(*args):
        copy = remote(*args)
        copy.start()
        sent.append(copy)

    loads = {}

    def load(name, src, dst):
        copy = pltpu.make_async_copy(src, dst, load_sem.at[len(loads)])
        copy.start()
        loads[name] = copy

    load("g", g_ref, gv)
    load("u", u_ref, uv)
    load("c", cot_ref, cv)
    load("x", x_ref, xv)
    load("wq", wd_ref.at[pl.ds(mult(y, q), q)], wq.at[y])
    for j in range(nf):
        load(f"wg{j}", wg_ref.at[pl.ds(j * q, q)], wcat.at[j, pl.ds(0, q)])
        load(f"wu{j}", wu_ref.at[pl.ds(j * q, q)], wcat.at[j, pl.ds(q, q)])

    barrier = pltpu.get_barrier_semaphore()
    near = [at(rz=rep(way * step)) for step in range(1, max(3, *STRIDES) + 1) for way in (1, -1)]
    near += [at(ry=lax.rem(y + step, nf)) for step in range(1, nf)]
    near += [at(rt=lax.rem(t + step, nt)) for step in range(1, nt)]
    for device in near:
        pl.semaphore_signal(barrier, inc=1, device_id=device, device_id_type=MESH)
    pl.semaphore_wait(barrier, len(near))

    far_a = wd_ref.at[pl.ds(pl.multiple_of(across * q, 16), top)]
    far_b = wd_ref.at[pl.ds(pl.multiple_of(across * q + top, 16), low)]
    send(far_a, relay_a, a2a_s.at[0], a2a_r.at[0], at(ry=right))
    send(far_b, relay_b, a2a_s.at[1], a2a_r.at[1], at(ry=left))
    send(wd_ref.at[pl.ds(mult(right, q), q)], wq.at[y], a2a_s.at[2], a2a_r.at[2], at(ry=right))
    send(wd_ref.at[pl.ds(mult(left, q), q)], wq.at[y], a2a_s.at[3], a2a_r.at[3], at(ry=left))

    loads["g"].wait()
    loads["u"].wait()
    step_rows = 16

    def factors(index, carry):
        span = pl.ds(pl.multiple_of(index * step_rows, step_rows), step_rows)
        gate = gv[span, :].astype(SINGLE)
        upper = uv[span, :].astype(SINGLE)
        sigma = 1.0 / (1.0 + jnp.exp(-gate))
        active = gate * sigma
        cu[span, :] = active
        hid[span, :] = (active * upper).astype(HALF)
        cg[span, :] = upper * sigma * (1.0 + gate * (1.0 - sigma))
        return carry

    lax.fori_loop(0, hunits // step_rows, factors, 0)

    place = lax.broadcasted_iota(jnp.int32, (width, width), 0)
    column = lax.broadcasted_iota(jnp.int32, (width, width), 1)
    bits = own.bit_length() - 1
    origin = (place & (own - 1)) * nr + (place >> bits)
    pick = jnp.where(column == origin, 1.0, 0.0).astype(HALF)
    loads["c"].wait()
    cp[...] = dot_nt(pick, cv[:, pl.ds(mult(y, width), width)]).astype(HALF)
    sets = [chain_refs[9 * n : 9 * n + 9] for n in range(len(STRIDES))]
    sets[0][0][...] = dot_nt(cp[...], hid[...]) * factor

    specs = [chains_of(nr, stride) for stride in STRIDES]
    clock = [0] * len(specs)

    def local(mine, owner):
        return mine[pl.ds(mult(owner, own), own), :]

    def tick(s):
        with jax.named_scope(f"tick#s={s}"):
            step(s)

    def sides(s, c, piece):
        _, _, _, side_src, side_dst, _, _, side_s, side_r = sets[s]
        count = side_count(nr, STRIDES[s])
        span = pl.ds(count // 2, count - count // 2) if piece == 0 else pl.ds(0, count // 2)
        for r in range(1, STRIDES[s]):
            yield r, side_src.at[c, r - 1, span], side_dst.at[c, r - 1, span], side_s.at[c, r - 1, piece], side_r.at[c, r - 1, piece]

    def launch_sides(s):
        mine, _, _, side_src, _, _, _, _, _ = sets[s]
        stride = STRIDES[s]
        count = side_count(nr, stride)
        for piece in (0, 1):
            for c, (way, far, _, _) in enumerate(specs[s]):
                for r in range(1, stride):
                    for m in range(count // 2, count) if piece == 0 else range(count // 2):
                        side_src[c, r - 1, m] = local(mine, rep(way * (stride * m + r))).astype(HALF)
            for c, (way, _, _, _) in enumerate(specs[s]):
                for r, src, dst, ssem, rsem in sides(s, c, piece):
                    send(src, dst, ssem, rsem, at(rz=rep(way * r)))

    def step(s):
        tau = clock[s]
        clock[s] += 1
        mine, stage, buf, _, side_dst, ssem, rsem, _, _ = sets[s]
        stride = STRIDES[s]
        count = side_count(nr, stride)
        for c, (way, far, links, delay) in enumerate(specs[s]):
            k = tau - delay
            m = links - k
            if tau == 1:
                for _, _, dst, _, rsem_side in sides(s, c, 0):
                    arrived(dst, rsem_side)
            if m == count // 2 - 1:
                for _, _, dst, _, rsem_side in sides(s, c, 1):
                    arrived(dst, rsem_side)
            if not 0 <= k <= links:
                continue
            if k > 0:
                arrived(buf.at[c, k - 1], rsem.at[c, k - 1])
            if k == links:
                continue
            total = local(mine, rep(way * stride * m))
            for r in range(1, stride):
                if stride * m + r <= far:
                    total = total + side_dst[c, r - 1, m].astype(SINGLE)
            if k == 0:
                src = stage.at[c]
            else:
                src = buf.at[c, k - 1]
                total = total + src[...].astype(SINGLE)
            src[...] = total.astype(HALF)
            send(src, buf.at[c, k], ssem.at[c, k], rsem.at[c, k], at(rz=rep(way * stride)))
        if tau == 0:
            launch_sides(s)

    def length(s):
        return max(links + delay for _, _, links, delay in specs[s])

    def total_of(s):
        mine, _, buf, _, side_dst, _, _, _, _ = sets[s]
        total = local(mine, z)
        for c, (_, _, links, _) in enumerate(specs[s]):
            total = total + buf[c, links - 1].astype(SINGLE)
            for r in range(1, STRIDES[s]):
                total = total + side_dst[c, r - 1, 0].astype(SINGLE)
        return total

    tick(0)

    loads["x"].wait()
    xp[...] = dot_nt(pick, xv[...]).astype(HALF)

    arrived(relay_a, a2a_r.at[0])
    send(relay_a, wq.at[left, pl.ds(0, top)], a2a_s.at[4], a2a_r.at[4], at(ry=right))
    arrived(relay_b, a2a_r.at[1])
    send(relay_b, wq.at[right, pl.ds(top, low)], a2a_s.at[5], a2a_r.at[5], at(ry=left))
    tick(0)

    def piece(j):
        return dot_nt(wq[j], cv[:, pl.ds(mult(j, width), width)])

    loads["wq"].wait()
    arrived(wq.at[left], a2a_r.at[2])
    arrived(wq.at[right], a2a_r.at[3])
    part = piece(y) + piece(left) + piece(right)
    arrived(wq.at[across, pl.ds(0, top)], a2a_r.at[4])
    arrived(wq.at[across, pl.ds(top, low)], a2a_r.at[5])
    hgb[y] = (part + piece(across)).astype(HALF)
    upper_rows, lower_rows = pl.ds(0, top), pl.ds(top, low)
    send(hgb.at[y, upper_rows], hgb.at[y, upper_rows], hg_s.at[0], hg_r.at[0], at(ry=right))
    send(hgb.at[y, lower_rows], hgb.at[y, lower_rows], hg_s.at[1], hg_r.at[1], at(ry=left))
    send(hgb.at[y, lower_rows], hgb.at[y, lower_rows], hg_s.at[2], hg_r.at[2], at(ry=right))
    send(hgb.at[y, upper_rows], hgb.at[y, upper_rows], hg_s.at[3], hg_r.at[3], at(ry=left))

    def quarter(i):
        j = order[i]
        span = pl.ds(mult(j, q), q)
        grad = hgb[j].astype(SINGLE)
        dall[i, 0:q, :] = (grad * cg[span, :]).astype(HALF)
        dall[i, q : 2 * q, :] = (grad * cu[span, :]).astype(HALF)
        sets[1 + i][0][...] = dot_nt(xp[...], dall[i]) * factor
        tick(1 + i)

    quarter(0)
    tick(0)
    arrived(hgb.at[left, upper_rows], hg_r.at[0])
    send(hgb.at[left, upper_rows], hgb.at[left, upper_rows], hg_s.at[4], hg_r.at[4], at(ry=right))
    arrived(hgb.at[right, lower_rows], hg_r.at[1])
    send(hgb.at[right, lower_rows], hgb.at[right, lower_rows], hg_s.at[5], hg_r.at[5], at(ry=left))
    tick(0)
    tick(1)
    arrived(hgb.at[left, lower_rows], hg_r.at[2])
    quarter(1)
    arrived(hgb.at[right, upper_rows], hg_r.at[3])
    quarter(2)
    tick(0)
    tick(1)
    arrived(hgb.at[across, upper_rows], hg_r.at[4])
    arrived(hgb.at[across, lower_rows], hg_r.at[5])
    quarter(3)

    for name in [f"w{kind}{j}" for kind in "gu" for j in range(nf)]:
        loads[name].wait()

    block = 128

    def terms(n):
        span = pl.ds(n * block, block)
        total = dot_tn(dall[0, :, span], wcat[order[0]])
        for i in range(1, nf):
            total = total + dot_tn(dall[i, :, span], wcat[order[i]])
        term[span, :] = total.astype(HALF)

    peers = [lax.rem(t + step, nt) for step in range(1, nt)]

    def terms_out():
        for n, peer in enumerate(peers):
            send(term.at[pl.ds(mult(peer, rows), rows)], parts.at[t], ti_s.at[n], ti_r.at[n], at(rt=peer))
        parts[t] = term[pl.ds(mult(t, rows), rows), :]

    def sources():
        return [lax.rem(t + nt - step, nt) for step in range(1, nt)]

    def terms_sum():
        for n, peer in enumerate(sources()):
            arrived(parts.at[peer], ti_r.at[n])
        total = parts[0].astype(SINGLE)
        for n in range(1, nt):
            total = total + parts[n].astype(SINGLE)
        res[...] = total.astype(HALF)
        for n, peer in enumerate(peers):
            send(res, gi_ref.at[t], to_s.at[n], to_r.at[n], at(rt=peer))
        pltpu.make_async_copy(res, gi_ref.at[t], out_sem).start()

    def terms_end():
        for n, peer in enumerate(sources()):
            arrived(gi_ref.at[peer], to_r.at[n])
        pltpu.make_async_copy(res, gi_ref.at[t], out_sem).wait()

    def exchange(slots, mine, count, base, device_of):
        slots[mine] = dmine[...]
        for step in range(1, count):
            n = base + step - 1
            send(dmine, slots.at[mine], m_s.at[n], m_r.at[n], device_of(lax.rem(mine + step, count)))

    def summed(slots, mine, count, base):
        for step in range(1, count):
            arrived(slots.at[lax.rem(mine + count - step, count)], m_r.at[base + step - 1])
        total = slots[0]
        for n in range(1, count):
            total = total + slots[n]
        return total

    group = 4
    inner, outer = lax.rem(z, group), z // group
    across_y = (dy, y, nf, 0)
    across_in = (dgroup, inner, group, nf - 1)
    across_out = (dfar, outer, nr // group, nf + group - 2)
    dscr = (dmine,)

    def down_first():
        total = total_of(0)
        gd_ref[...] = total
        dmine[...] = jnp.sum(total * total, axis=0, keepdims=True)
        exchange(*across_y, lambda p: at(ry=p))

    def down_second():
        nvalue = summed(*across_y)
        dgroup[inner] = nvalue
        for step in range(1, group):
            n = nf - 1 + step - 1
            peer = lax.rem(inner + step, group)
            send(dgroup.at[inner], dgroup.at[inner], m_s.at[n], m_r.at[n], at(rz=outer * group + peer))

    def down_third():
        dfar[outer] = summed(*across_in)
        count = nr // group
        for step in range(1, count):
            n = nf + group - 2 + step - 1
            peer = lax.rem(outer + step, count)
            send(dfar.at[outer], dfar.at[outer], m_s.at[n], m_r.at[n], at(rz=peer * group + inner))

    def down_last():
        dn_ref[...] = summed(*across_out)

    blocks = tokens // block
    input_stage = [functools.partial(terms, n) for n in range(blocks)]
    input_stage += [terms_out] + [lambda: None] * WAITS + [terms_sum]
    down_stage = [down_first, down_second, down_third]
    n_tick = 0
    while any(clock[s] <= length(s) for s in ROUND):
        n_tick += 1
        for s in ROUND:
            if clock[s] <= length(s):
                tick(s)
        for _ in range(PER_TICK):
            if input_stage:
                input_stage.pop(0)()
        if clock[0] > length(0) and down_stage:
            down_stage.pop(0)()
    for stage in input_stage + down_stage:
        stage()

    for i in range(nf):
        fin[order[i]] = total_of(1 + i)
    gate_total = jnp.zeros((own, 1), SINGLE)
    up_total = jnp.zeros((own, 1), SINGLE)
    for j in range(nf):
        gate_part, up_part = fin[j, :, 0:q], fin[j, :, q : 2 * q]
        gg_ref[:, j * q : (j + 1) * q] = gate_part
        gu_ref[:, j * q : (j + 1) * q] = up_part
        gate_total = gate_total + jnp.sum(gate_part * gate_part, axis=1, keepdims=True)
        up_total = up_total + jnp.sum(up_part * up_part, axis=1, keepdims=True)
    lane = lax.broadcasted_iota(jnp.int32, (own, 128), 1)
    nvec[...] = jnp.where(lane < 64, gate_total, up_total)
    nrecv[t] = nvec[...]
    for n, peer in enumerate(peers):
        send(nvec, nrecv.at[t], n_s.at[n], n_r.at[n], at(rt=peer))
    terms_end()
    for n, peer in enumerate(sources()):
        arrived(nrecv.at[peer], n_r.at[n])
    norms = nrecv[0]
    for n in range(1, nt):
        norms = norms + nrecv[n]
    turned = norms.T
    gn_ref[...] = turned[0:1, :]
    un_ref[...] = turned[64:65, :]
    down_last()
    for copy in sent:
        copy.wait_send()


def finish(gi_ref, gg_ref, gu_ref, gd_ref, gn_ref, un_ref, dn_ref, *out):
    gi_out, gg_out, gu_out, gd_out, gn_out, un_out, dn_out = out
    gi_out[...] = gi_ref[...]
    for src, dst in ((gg_ref, gg_out), (gu_ref, gu_out), (gd_ref, gd_out)):
        dst[...] = src[...].reshape(dst.shape)
    gn_out[...] = gn_ref[...]
    un_out[...] = un_ref[...]
    dn_out[...] = dn_ref[0, :]


def on_device(inputs, gate_pre, up_pre, cotangent, w_gate, w_up, w_down):
    nr, nf, nt = (lax.axis_size(name) for name in ("rep", "fs", "tp"))
    tokens, width = inputs.shape
    hunits = w_gate.shape[1]
    q, own, rows = hunits // nf, width // nr, tokens // nt
    top = -(-q // 32) * 16
    features = cotangent.shape[1]
    vmem, dma = pltpu.VMEM, pltpu.SemaphoreType.DMA
    any_space = pl.BlockSpec(memory_space=pl.ANY)
    in_vmem = pl.BlockSpec(memory_space=pltpu.VMEM)
    shape = jax.ShapeDtypeStruct
    chain_scratch = []
    for stride, lanes in zip(STRIDES, (hunits,) + (2 * q,) * nf):
        links = nr // 2 // stride
        side = (2, max(stride - 1, 1), side_count(nr, stride))
        chain_scratch += [
            vmem((width, lanes), SINGLE),
            vmem((2, own, lanes), HALF),
            vmem((2, links, own, lanes), HALF),
            vmem((*side, own, lanes), HALF),
            vmem((*side, own, lanes), HALF),
            dma((2, links)),
            dma((2, links)),
            dma((2, side[1], 2)),
            dma((2, side[1], 2)),
        ]
    small = (nf - 1) + 3 + (nr // 4 - 1)
    gi, gg, gu, gd, gn, un, dn = pl.pallas_call(
        functools.partial(kernel, (nr, nf, nt)),
        out_shape=(
            shape((nt, rows, width), HALF),
            shape((own, hunits), SINGLE),
            shape((own, hunits), SINGLE),
            shape((own, hunits), SINGLE),
            shape((1, own), SINGLE),
            shape((1, own), SINGLE),
            shape((1, hunits), SINGLE),
        ),
        in_specs=[any_space] * 7,
        out_specs=(any_space,) + (in_vmem,) * 6,
        scratch_shapes=[
            vmem((tokens, width), HALF),
            vmem((hunits, tokens), HALF),
            vmem((hunits, tokens), HALF),
            vmem((tokens, features), HALF),
            vmem((nf, 2 * q, width), HALF),
            vmem((nf, q, width), HALF),
            vmem((top, width), HALF),
            vmem((q - top, width), HALF),
            vmem((nf, q, tokens), HALF),
            vmem((hunits, tokens), SINGLE),
            vmem((hunits, tokens), SINGLE),
            vmem((hunits, tokens), HALF),
            vmem((width, tokens), HALF),
            vmem((width, tokens), HALF),
            vmem((nf, 2 * q, tokens), HALF),
            vmem((nf, own, 2 * q), SINGLE),
            vmem((tokens, width), HALF),
            vmem((nt, rows, width), HALF),
            vmem((rows, width), HALF),
            vmem((own, 128), SINGLE),
            vmem((nt, own, 128), SINGLE),
            vmem((1, hunits), SINGLE),
            vmem((nf, 1, hunits), SINGLE),
            vmem((4, 1, hunits), SINGLE),
            vmem((nr // 4, 1, hunits), SINGLE),
            dma((5 + 2 * nf,)),
            dma((6,)),
            dma((6,)),
            dma((6,)),
            dma((6,)),
            dma((nt - 1,)),
            dma((nt - 1,)),
            dma((nt - 1,)),
            dma((nt - 1,)),
            dma((nt - 1,)),
            dma((nt - 1,)),
            dma((small,)),
            dma((small,)),
            dma(()),
            *chain_scratch,
        ],
        compiler_params=pltpu.CompilerParams(
            collective_id=0, has_side_effects=True, vmem_limit_bytes=56 * 2**20
        ),
    )(inputs, gate_pre.T, up_pre.T, cotangent, w_gate.T, w_up.T, w_down)
    gi, gg, gu, gd, gn, un, dn = pl.pallas_call(
        finish,
        out_shape=(
            shape((nt, rows, width), HALF),
            shape((own, 1, hunits), SINGLE),
            shape((own, 1, hunits), SINGLE),
            shape((own, 1, hunits), SINGLE),
            shape((1, own), SINGLE),
            shape((1, own), SINGLE),
            shape((hunits,), SINGLE),
        ),
        in_specs=[in_vmem] * 7,
        out_specs=(in_vmem,) * 7,
    )(gi, gg, gu, gd, gn, un, dn)
    return (
        gi.reshape(tokens, width),
        gg,
        gu,
        gd.transpose(2, 0, 1),
        gn.reshape(own, 1),
        un.reshape(own, 1),
        dn,
    )


def solution(mesh):
    placed = (
        P("rep", "fs"),
        P("rep", "tp"),
        P("rep", "tp"),
        P("rep", None),
        P("fs", "tp"),
        P("fs", "tp"),
        P("tp", "fs"),
    )
    return jax.shard_map(
        on_device,
        mesh=mesh,
        in_specs=placed,
        out_specs=(
            P("rep", "fs"),
            P("fs", "rep", "tp"),
            P("fs", "rep", "tp"),
            P("tp", "fs", "rep"),
            P("fs", "rep"),
            P("fs", "rep"),
            P("tp"),
        ),
        check_vma=False,
    )
```

```python
import functools

import jax
import jax.numpy as jnp
from jax import lax
from jax.experimental import pallas as pl
from jax.experimental.pallas import tpu as pltpu
from jax.sharding import PartitionSpec as P

MESH = pl.DeviceIdType.MESH
SINGLE = jnp.float32
HALF = jnp.bfloat16
STRIDES = (2, 2, 2, 2, 2)
PER_TICK = 2
WAITS = 5
ROUND = (1, 2, 3, 4, 0)
PIECE = (2, 4, 1, 1, 1)
LEAD = (4, 8, 1, 1, 1)


def dot_nt(a, b):
    return lax.dot_general(a, b, (((1,), (1,)), ((), ())), preferred_element_type=SINGLE)


def dot_tn(a, b):
    return lax.dot_general(a, b, (((0,), (0,)), ((), ())), preferred_element_type=SINGLE)


def chains_of(groups, stride):
    half = groups // 2
    found = []
    for way, far in ((1, half), (-1, groups - 1 - half)):
        links = far // stride
        found.append((way, far, links, 0 if links * stride == far else 1))
    return found


def side_count(groups, stride):
    return (groups // 2 - 1) // stride + 1


def kernel(
    sizes,
    x_ref, g_ref, u_ref, cot_ref, wg_ref, wu_ref, wd_ref,
    gi_ref, gg_ref, gu_ref, gd_ref, gn_ref, un_ref, dn_ref,
    xv, gv, uv, cv, wv, wcat, wq, relay_a, relay_b, hgb, cg, cu, hid, xp, cp, dall,
    fin, term, parts, res,
    nvec, nrecv, dnear, dfar,
    load_sem, a2a_s, a2a_r, hg_s, hg_r,
    ti_s, ti_r, to_s, to_r, n_s, n_r, m_s, m_r, f_s, f_r, out_sem, *chain_refs,
):
    nr, nf, nt = sizes
    tokens, width = xv.shape
    hunits = gv.shape[0]
    q = hunits // nf
    own = width // nr
    top = -(-q // 32) * 16
    low = q - top
    rows = tokens // nt
    factor = float(tokens * nr) ** -0.5
    z, y, t = (lax.axis_index(name) for name in ("rep", "fs", "tp"))
    right, left, across = (lax.rem(y + step, nf) for step in (1, nf - 1, nf // 2))
    order = (y, left, right, across)

    def rep(step):
        return lax.rem(z + step + nr, nr)

    def at(rz=None, ry=None, rt=None):
        return (z if rz is None else rz, y if ry is None else ry, t if rt is None else rt)

    def remote(src, dst, ssem, rsem, device):
        return pltpu.make_async_remote_copy(
            src_ref=src, dst_ref=dst, send_sem=ssem, recv_sem=rsem, device_id=device, device_id_type=MESH
        )

    def arrived(ref, rsem):
        remote(ref, ref, rsem, rsem, at(ry=right)).wait_recv()

    def mult(value, by):
        return pl.multiple_of(value * by, by)

    sent = []

    def send(*args):
        copy = remote(*args)
        copy.start()
        sent.append(copy)

    loads = {}

    def load(name, src, dst):
        copy = pltpu.make_async_copy(src, dst, load_sem.at[len(loads)])
        copy.start()
        loads[name] = copy

    load("w", wd_ref, wv)
    load("g", g_ref, gv)
    load("u", u_ref, uv)
    load("c", cot_ref, cv)
    load("x", x_ref, xv)
    load("wq", wd_ref.at[pl.ds(mult(y, q), q)], wq.at[y])
    for j in range(nf):
        load(f"wg{j}", wg_ref.at[pl.ds(j * q, q)], wcat.at[j, pl.ds(0, q)])
        load(f"wu{j}", wu_ref.at[pl.ds(j * q, q)], wcat.at[j, pl.ds(q, q)])

    barrier = pltpu.get_barrier_semaphore()
    near = [at(rz=rep(way * step)) for step in range(1, max(2, *STRIDES) + 1) for way in (1, -1)]
    near += [at(ry=lax.rem(y + step, nf)) for step in range(1, nf)]
    near += [at(rt=lax.rem(t + step, nt)) for step in range(1, nt)]
    for device in near:
        pl.semaphore_signal(barrier, inc=1, device_id=device, device_id_type=MESH)
    loads["g"].wait()
    loads["u"].wait()
    step_rows = 16

    def factors(index, carry):
        span = pl.ds(pl.multiple_of(index * step_rows, step_rows), step_rows)
        gate = gv[span, :].astype(SINGLE)
        upper = uv[span, :].astype(SINGLE)
        sigma = 1.0 / (1.0 + jnp.exp(-gate))
        active = gate * sigma
        cu[span, :] = active
        hid[span, :] = (active * upper).astype(HALF)
        cg[span, :] = upper * sigma * (1.0 + gate * (1.0 - sigma))
        return carry

    lax.fori_loop(0, hunits // step_rows, factors, 0)

    pl.semaphore_wait(barrier, len(near))

    loads["w"].wait()
    far_a = wv.at[pl.ds(pl.multiple_of(across * q, 16), top)]
    far_b = wv.at[pl.ds(pl.multiple_of(across * q + top, 16), low)]
    send(far_a, relay_a, a2a_s.at[0], a2a_r.at[0], at(ry=right))
    send(far_b, relay_b, a2a_s.at[1], a2a_r.at[1], at(ry=left))
    send(wv.at[pl.ds(mult(right, q), q)], wq.at[y], a2a_s.at[2], a2a_r.at[2], at(ry=right))
    send(wv.at[pl.ds(mult(left, q), q)], wq.at[y], a2a_s.at[3], a2a_r.at[3], at(ry=left))

    place = lax.broadcasted_iota(jnp.int32, (width, width), 0)
    column = lax.broadcasted_iota(jnp.int32, (width, width), 1)
    bits = own.bit_length() - 1
    origin = (place & (own - 1)) * nr + (place >> bits)
    pick = jnp.where(column == origin, 1.0, 0.0).astype(HALF)
    loads["c"].wait()
    cp[...] = dot_nt(pick, cv[:, pl.ds(mult(y, width), width)]).astype(HALF)
    sets = [chain_refs[9 * n : 9 * n + 9] for n in range(len(STRIDES))]
    sets[0][0][...] = dot_nt(cp[...], hid[...]) * factor

    specs = [chains_of(nr, stride) for stride in STRIDES]
    clock = [0] * len(specs)

    def local(mine, owner):
        return mine[pl.ds(mult(owner, own), own), :]

    def tick(s):
        with jax.named_scope(f"tick#s={s}"):
            step(s)

    def side_span(s, piece):
        count, size = side_count(nr, STRIDES[s]), PIECE[s]
        return range(count - size * (piece + 1), count - size * piece)

    def sides(s, c, piece):
        _, _, _, side_src, side_dst, _, _, side_s, side_r = sets[s]
        span = pl.ds(side_span(s, piece).start, PIECE[s])
        for r in range(1, STRIDES[s]):
            yield r, side_src.at[c, r - 1, span], side_dst.at[c, r - 1, span], side_s.at[c, r - 1, piece], side_r.at[c, r - 1, piece]

    def launch_sides(s, piece):
        mine, _, _, side_src, _, _, _, _, _ = sets[s]
        stride = STRIDES[s]
        for c, (way, _, _, _) in enumerate(specs[s]):
            for r in range(1, stride):
                for m in side_span(s, piece):
                    side_src[c, r - 1, m] = local(mine, rep(way * (stride * m + r))).astype(HALF)
        for c, (way, _, _, _) in enumerate(specs[s]):
            for r, src, dst, ssem, rsem in sides(s, c, piece):
                send(src, dst, ssem, rsem, at(rz=rep(way * r)))

    def launch_due(s, tau):
        if STRIDES[s] > 1:
            for piece in range(side_count(nr, STRIDES[s]) // PIECE[s]):
                if tau == max(0, 1 + PIECE[s] * piece - LEAD[s]):
                    launch_sides(s, piece)

    def step(s):
        tau = clock[s]
        clock[s] += 1
        mine, stage, buf, _, side_dst, ssem, rsem, _, _ = sets[s]
        stride = STRIDES[s]
        count, size = side_count(nr, stride), PIECE[s]
        if tau > 0:
            launch_due(s, tau)
        for c, (way, far, links, delay) in enumerate(specs[s]):
            k = tau - delay
            m = links - k
            if stride > 1 and tau % size == 1 % size and 1 <= tau <= count:
                for _, _, dst, _, rsem_side in sides(s, c, (tau - 1) // size):
                    arrived(dst, rsem_side)
            if not 0 <= k <= links:
                continue
            if k > 0:
                arrived(buf.at[c, k - 1], rsem.at[c, k - 1])
            if k == links:
                continue
            total = local(mine, rep(way * stride * m))
            for r in range(1, stride):
                if stride * m + r <= far:
                    total = total + side_dst[c, r - 1, m].astype(SINGLE)
            if k == 0:
                src = stage.at[c]
            else:
                src = buf.at[c, k - 1]
                total = total + src[...].astype(SINGLE)
            src[...] = total.astype(HALF)
            send(src, buf.at[c, k], ssem.at[c, k], rsem.at[c, k], at(rz=rep(way * stride)))
        if tau == 0:
            launch_due(s, tau)

    def length(s):
        return max(links + delay for _, _, links, delay in specs[s])

    def total_of(s):
        mine, _, buf, _, side_dst, _, _, _, _ = sets[s]
        total = local(mine, z)
        for c, (_, _, links, _) in enumerate(specs[s]):
            total = total + buf[c, links - 1].astype(SINGLE)
            for r in range(1, STRIDES[s]):
                total = total + side_dst[c, r - 1, 0].astype(SINGLE)
        return total

    tick(0)

    loads["x"].wait()
    xp[...] = dot_nt(pick, xv[...]).astype(HALF)

    arrived(relay_a, a2a_r.at[0])
    send(relay_a, wq.at[left, pl.ds(0, top)], a2a_s.at[4], a2a_r.at[4], at(ry=right))
    arrived(relay_b, a2a_r.at[1])
    send(relay_b, wq.at[right, pl.ds(top, low)], a2a_s.at[5], a2a_r.at[5], at(ry=left))
    tick(0)

    def piece(j):
        return dot_nt(wq[j], cv[:, pl.ds(mult(j, width), width)])

    loads["wq"].wait()
    arrived(wq.at[left], a2a_r.at[2])
    arrived(wq.at[right], a2a_r.at[3])
    part = piece(y) + piece(left) + piece(right)
    arrived(wq.at[across, pl.ds(0, top)], a2a_r.at[4])
    arrived(wq.at[across, pl.ds(top, low)], a2a_r.at[5])
    hgb[y] = (part + piece(across)).astype(HALF)
    upper_rows, lower_rows = pl.ds(0, top), pl.ds(top, low)
    send(hgb.at[y, upper_rows], hgb.at[y, upper_rows], hg_s.at[0], hg_r.at[0], at(ry=right))
    send(hgb.at[y, lower_rows], hgb.at[y, lower_rows], hg_s.at[1], hg_r.at[1], at(ry=left))
    send(hgb.at[y, lower_rows], hgb.at[y, lower_rows], hg_s.at[2], hg_r.at[2], at(ry=right))
    send(hgb.at[y, upper_rows], hgb.at[y, upper_rows], hg_s.at[3], hg_r.at[3], at(ry=left))

    def quarter(i):
        j = order[i]
        span = pl.ds(mult(j, q), q)
        grad = hgb[j].astype(SINGLE)
        dall[i, 0:q, :] = (grad * cg[span, :]).astype(HALF)
        dall[i, q : 2 * q, :] = (grad * cu[span, :]).astype(HALF)
        sets[1 + i][0][...] = dot_nt(xp[...], dall[i]) * factor
        tick(1 + i)

    quarter(0)
    tick(0)
    arrived(hgb.at[left, upper_rows], hg_r.at[0])
    send(hgb.at[left, upper_rows], hgb.at[left, upper_rows], hg_s.at[4], hg_r.at[4], at(ry=right))
    arrived(hgb.at[right, lower_rows], hg_r.at[1])
    send(hgb.at[right, lower_rows], hgb.at[right, lower_rows], hg_s.at[5], hg_r.at[5], at(ry=left))
    tick(0)
    tick(1)
    arrived(hgb.at[left, lower_rows], hg_r.at[2])
    quarter(1)
    arrived(hgb.at[right, upper_rows], hg_r.at[3])
    quarter(2)
    arrived(hgb.at[across, upper_rows], hg_r.at[4])
    arrived(hgb.at[across, lower_rows], hg_r.at[5])
    quarter(3)
    tick(0)

    for name in [f"w{kind}{j}" for kind in "gu" for j in range(nf)]:
        loads[name].wait()

    block = 128

    def terms(n):
        span = pl.ds(n * block, block)
        total = dot_tn(dall[0, :, span], wcat[order[0]])
        for i in range(1, nf):
            total = total + dot_tn(dall[i, :, span], wcat[order[i]])
        term[span, :] = total.astype(HALF)

    peers = [lax.rem(t + step, nt) for step in range(1, nt)]

    def terms_out():
        for n, peer in enumerate(peers):
            send(term.at[pl.ds(mult(peer, rows), rows)], parts.at[t], ti_s.at[n], ti_r.at[n], at(rt=peer))
        parts[t] = term[pl.ds(mult(t, rows), rows), :]

    def sources():
        return [lax.rem(t + nt - step, nt) for step in range(1, nt)]

    def terms_sum():
        for n, peer in enumerate(sources()):
            arrived(parts.at[peer], ti_r.at[n])
        total = parts[0].astype(SINGLE)
        for n in range(1, nt):
            total = total + parts[n].astype(SINGLE)
        res[...] = total.astype(HALF)
        for n, peer in enumerate(peers):
            send(res, gi_ref.at[t], to_s.at[n], to_r.at[n], at(rt=peer))
        pltpu.make_async_copy(res, gi_ref.at[t], out_sem).start()

    def terms_end():
        for n, peer in enumerate(sources()):
            arrived(gi_ref.at[peer], to_r.at[n])
        pltpu.make_async_copy(res, gi_ref.at[t], out_sem).wait()

    group = 4
    inner, outer = lax.rem(z, group), z // group
    count = nr // group

    def down_first():
        total = total_of(0)
        gd_ref[...] = total
        dnear[inner, y] = jnp.sum(total * total, axis=0, keepdims=True)
        for n in range(1, group * nf):
            by_z, by_y = n // nf, n % nf
            device = at(rz=outer * group + lax.rem(inner + by_z, group), ry=lax.rem(y + by_y, nf))
            send(dnear.at[inner, y], dnear.at[inner, y], m_s.at[n - 1], m_r.at[n - 1], device)

    def down_second():
        for n in range(1, group * nf):
            by_z, by_y = n // nf, n % nf
            place = dnear.at[lax.rem(inner + group - by_z, group), lax.rem(y + nf - by_y, nf)]
            arrived(place, m_r.at[n - 1])
        total = dnear[0, 0]
        for n in range(1, group * nf):
            total = total + dnear[n // nf, n % nf]
        dfar[outer] = total
        for n in range(1, count):
            device = at(rz=lax.rem(outer + n, count) * group + inner)
            send(dfar.at[outer], dfar.at[outer], f_s.at[n - 1], f_r.at[n - 1], device)

    def down_last():
        for n in range(1, count):
            arrived(dfar.at[lax.rem(outer + count - n, count)], f_r.at[n - 1])
        total = dfar[0]
        for n in range(1, count):
            total = total + dfar[n]
        dn_ref[...] = total

    blocks = tokens // block
    input_stage = [functools.partial(terms, n) for n in range(blocks)]
    input_stage += [terms_out] + [lambda: None] * WAITS + [terms_sum]
    down_stage = [down_first, down_second]
    n_tick = 0
    while any(clock[s] <= length(s) for s in ROUND):
        n_tick += 1
        for s in ROUND:
            if clock[s] <= length(s):
                tick(s)
        for _ in range(PER_TICK):
            if input_stage:
                input_stage.pop(0)()
        if clock[0] > length(0) and down_stage:
            down_stage.pop(0)()
    for stage in input_stage + down_stage:
        stage()

    for i in range(nf):
        fin[order[i]] = total_of(1 + i)
    gate_total = jnp.zeros((own, 1), SINGLE)
    up_total = jnp.zeros((own, 1), SINGLE)
    for j in range(nf):
        gate_part, up_part = fin[j, :, 0:q], fin[j, :, q : 2 * q]
        gg_ref[:, j * q : (j + 1) * q] = gate_part
        gu_ref[:, j * q : (j + 1) * q] = up_part
        gate_total = gate_total + jnp.sum(gate_part * gate_part, axis=1, keepdims=True)
        up_total = up_total + jnp.sum(up_part * up_part, axis=1, keepdims=True)
    lane = lax.broadcasted_iota(jnp.int32, (own, 128), 1)
    nvec[...] = jnp.where(lane < 64, gate_total, up_total)
    nrecv[t] = nvec[...]
    for n, peer in enumerate(peers):
        send(nvec, nrecv.at[t], n_s.at[n], n_r.at[n], at(rt=peer))
    terms_end()
    for n, peer in enumerate(sources()):
        arrived(nrecv.at[peer], n_r.at[n])
    norms = nrecv[0]
    for n in range(1, nt):
        norms = norms + nrecv[n]
    turned = norms.T
    gn_ref[...] = turned[0:1, :]
    un_ref[...] = turned[64:65, :]
    down_last()
    for copy in sent:
        copy.wait_send()


def finish(gi_ref, gg_ref, gu_ref, gd_ref, gn_ref, un_ref, dn_ref, *out):
    gi_out, gg_out, gu_out, gd_out, gn_out, un_out, dn_out = out
    gi_out[...] = gi_ref[...]
    for src, dst in ((gg_ref, gg_out), (gu_ref, gu_out), (gd_ref, gd_out)):
        dst[...] = src[...].reshape(dst.shape)
    gn_out[...] = gn_ref[...]
    un_out[...] = un_ref[...]
    dn_out[...] = dn_ref[0, :]


def on_device(inputs, gate_pre, up_pre, cotangent, w_gate, w_up, w_down):
    nr, nf, nt = (lax.axis_size(name) for name in ("rep", "fs", "tp"))
    tokens, width = inputs.shape
    hunits = w_gate.shape[1]
    q, own, rows = hunits // nf, width // nr, tokens // nt
    top = -(-q // 32) * 16
    features = cotangent.shape[1]
    vmem, dma = pltpu.VMEM, pltpu.SemaphoreType.DMA
    any_space = pl.BlockSpec(memory_space=pl.ANY)
    in_vmem = pl.BlockSpec(memory_space=pltpu.VMEM)
    shape = jax.ShapeDtypeStruct
    chain_scratch = []
    for stride, size, lanes in zip(STRIDES, PIECE, (hunits,) + (2 * q,) * nf):
        links = nr // 2 // stride
        side = (2, max(stride - 1, 1), side_count(nr, stride))
        chain_scratch += [
            vmem((width, lanes), SINGLE),
            vmem((2, own, lanes), HALF),
            vmem((2, links, own, lanes), HALF),
            vmem((*side, own, lanes), HALF),
            vmem((*side, own, lanes), HALF),
            dma((2, links)),
            dma((2, links)),
            dma((2, side[1], side[2] // size)),
            dma((2, side[1], side[2] // size)),
        ]
    gi, gg, gu, gd, gn, un, dn = pl.pallas_call(
        functools.partial(kernel, (nr, nf, nt)),
        out_shape=(
            shape((nt, rows, width), HALF),
            shape((own, hunits), SINGLE),
            shape((own, hunits), SINGLE),
            shape((own, hunits), SINGLE),
            shape((1, own), SINGLE),
            shape((1, own), SINGLE),
            shape((1, hunits), SINGLE),
        ),
        in_specs=[any_space] * 7,
        out_specs=(any_space,) + (in_vmem,) * 6,
        scratch_shapes=[
            vmem((tokens, width), HALF),
            vmem((hunits, tokens), HALF),
            vmem((hunits, tokens), HALF),
            vmem((tokens, features), HALF),
            vmem((hunits, width), HALF),
            vmem((nf, 2 * q, width), HALF),
            vmem((nf, q, width), HALF),
            vmem((top, width), HALF),
            vmem((q - top, width), HALF),
            vmem((nf, q, tokens), HALF),
            vmem((hunits, tokens), SINGLE),
            vmem((hunits, tokens), SINGLE),
            vmem((hunits, tokens), HALF),
            vmem((width, tokens), HALF),
            vmem((width, tokens), HALF),
            vmem((nf, 2 * q, tokens), HALF),
            vmem((nf, own, 2 * q), SINGLE),
            vmem((tokens, width), HALF),
            vmem((nt, rows, width), HALF),
            vmem((rows, width), HALF),
            vmem((own, 128), SINGLE),
            vmem((nt, own, 128), SINGLE),
            vmem((4, nf, 1, hunits), SINGLE),
            vmem((nr // 4, 1, hunits), SINGLE),
            dma((6 + 2 * nf,)),
            dma((6,)),
            dma((6,)),
            dma((6,)),
            dma((6,)),
            dma((nt - 1,)),
            dma((nt - 1,)),
            dma((nt - 1,)),
            dma((nt - 1,)),
            dma((nt - 1,)),
            dma((nt - 1,)),
            dma((4 * nf - 1,)),
            dma((4 * nf - 1,)),
            dma((nr // 4 - 1,)),
            dma((nr // 4 - 1,)),
            dma(()),
            *chain_scratch,
        ],
        compiler_params=pltpu.CompilerParams(
            collective_id=0, has_side_effects=True, vmem_limit_bytes=56 * 2**20
        ),
    )(inputs, gate_pre.T, up_pre.T, cotangent, w_gate.T, w_up.T, w_down)
    gi, gg, gu, gd, gn, un, dn = pl.pallas_call(
        finish,
        out_shape=(
            shape((nt, rows, width), HALF),
            shape((own, 1, hunits), SINGLE),
            shape((own, 1, hunits), SINGLE),
            shape((own, 1, hunits), SINGLE),
            shape((1, own), SINGLE),
            shape((1, own), SINGLE),
            shape((hunits,), SINGLE),
        ),
        in_specs=[in_vmem] * 7,
        out_specs=(in_vmem,) * 7,
    )(gi, gg, gu, gd, gn, un, dn)
    return (
        gi.reshape(tokens, width),
        gg,
        gu,
        gd.transpose(2, 0, 1),
        gn.reshape(own, 1),
        un.reshape(own, 1),
        dn,
    )


def solution(mesh):
    placed = (
        P("rep", "fs"),
        P("rep", "tp"),
        P("rep", "tp"),
        P("rep", None),
        P("fs", "tp"),
        P("fs", "tp"),
        P("tp", "fs"),
    )
    return jax.shard_map(
        on_device,
        mesh=mesh,
        in_specs=placed,
        out_specs=(
            P("rep", "fs"),
            P("fs", "rep", "tp"),
            P("fs", "rep", "tp"),
            P("tp", "fs", "rep"),
            P("fs", "rep"),
            P("fs", "rep"),
            P("tp"),
        ),
        check_vma=False,
    )
```

```python
import functools

import jax
import jax.numpy as jnp
from jax import lax
from jax.experimental import pallas as pl
from jax.experimental.pallas import tpu as pltpu
from jax.sharding import PartitionSpec as P

MESH = pl.DeviceIdType.MESH
SINGLE = jnp.float32
HALF = jnp.bfloat16
STRIDES = (2, 2, 2, 2, 2)
PER_TICK = 2
WAITS = 5
ROUND = (1, 2, 3, 4, 0)
PIECE = (2, 2, 1, 1, 1)
LEAD = (4, 3, 1, 1, 1)


def dot_nt(a, b):
    return lax.dot_general(a, b, (((1,), (1,)), ((), ())), preferred_element_type=SINGLE)


def dot_tn(a, b):
    return lax.dot_general(a, b, (((0,), (0,)), ((), ())), preferred_element_type=SINGLE)


def chains_of(groups, stride):
    half = groups // 2
    found = []
    for way, far in ((1, half), (-1, groups - 1 - half)):
        links = far // stride
        found.append((way, far, links, 0 if links * stride == far else 1))
    return found


def side_count(groups, stride):
    return (groups // 2 - 1) // stride + 1


def kernel(
    sizes,
    x_ref, g_ref, u_ref, cot_ref, wg_ref, wu_ref, wd_ref,
    gi_ref, gg_ref, gu_ref, gd_ref, gn_ref, un_ref, dn_ref,
    xv, gv, uv, cv, wv, wcat, wq, relay_a, relay_b, hgb, cg, cu, hid, xp, cp, dall,
    fin, term, parts, res,
    nvec, nrecv, dnear, dfar,
    load_sem, a2a_s, a2a_r, hg_s, hg_r,
    ti_s, ti_r, to_s, to_r, n_s, n_r, m_s, m_r, f_s, f_r, out_sem, *chain_refs,
):
    nr, nf, nt = sizes
    tokens, width = xv.shape
    hunits = gv.shape[0]
    q = hunits // nf
    own = width // nr
    top = -(-q // 32) * 16
    low = q - top
    rows = tokens // nt
    factor = float(tokens * nr) ** -0.5
    z, y, t = (lax.axis_index(name) for name in ("rep", "fs", "tp"))
    right, left, across = (lax.rem(y + step, nf) for step in (1, nf - 1, nf // 2))
    order = (y, left, right, across)

    def rep(step):
        return lax.rem(z + step + nr, nr)

    def at(rz=None, ry=None, rt=None):
        return (z if rz is None else rz, y if ry is None else ry, t if rt is None else rt)

    def remote(src, dst, ssem, rsem, device):
        return pltpu.make_async_remote_copy(
            src_ref=src, dst_ref=dst, send_sem=ssem, recv_sem=rsem, device_id=device, device_id_type=MESH
        )

    def arrived(ref, rsem):
        remote(ref, ref, rsem, rsem, at(ry=right)).wait_recv()

    def mult(value, by):
        return pl.multiple_of(value * by, by)

    sent = []

    def send(*args):
        copy = remote(*args)
        copy.start()
        sent.append(copy)

    loads = {}

    def load(name, src, dst):
        copy = pltpu.make_async_copy(src, dst, load_sem.at[len(loads)])
        copy.start()
        loads[name] = copy

    load("w", wd_ref, wv)
    load("g", g_ref, gv)
    load("u", u_ref, uv)
    load("c", cot_ref, cv)
    load("x", x_ref, xv)
    load("wq", wd_ref.at[pl.ds(mult(y, q), q)], wq.at[y])
    for j in range(nf):
        load(f"wg{j}", wg_ref.at[pl.ds(j * q, q)], wcat.at[j, pl.ds(0, q)])
        load(f"wu{j}", wu_ref.at[pl.ds(j * q, q)], wcat.at[j, pl.ds(q, q)])

    barrier = pltpu.get_barrier_semaphore()
    near = [at(rz=rep(way * step)) for step in range(1, max(2, *STRIDES) + 1) for way in (1, -1)]
    near += [at(ry=lax.rem(y + step, nf)) for step in range(1, nf)]
    near += [at(rt=lax.rem(t + step, nt)) for step in range(1, nt)]
    for device in near:
        pl.semaphore_signal(barrier, inc=1, device_id=device, device_id_type=MESH)
    loads["g"].wait()
    loads["u"].wait()
    step_rows = 16

    def factors(index, carry):
        span = pl.ds(pl.multiple_of(index * step_rows, step_rows), step_rows)
        gate = gv[span, :].astype(SINGLE)
        upper = uv[span, :].astype(SINGLE)
        sigma = 1.0 / (1.0 + jnp.exp(-gate))
        active = gate * sigma
        cu[span, :] = active
        hid[span, :] = (active * upper).astype(HALF)
        cg[span, :] = upper * sigma * (1.0 + gate * (1.0 - sigma))
        return carry

    lax.fori_loop(0, hunits // step_rows, factors, 0)

    pl.semaphore_wait(barrier, len(near))

    loads["w"].wait()
    far_a = wv.at[pl.ds(pl.multiple_of(across * q, 16), top)]
    far_b = wv.at[pl.ds(pl.multiple_of(across * q + top, 16), low)]
    send(far_a, relay_a, a2a_s.at[0], a2a_r.at[0], at(ry=right))
    send(far_b, relay_b, a2a_s.at[1], a2a_r.at[1], at(ry=left))
    send(wv.at[pl.ds(mult(right, q), q)], wq.at[y], a2a_s.at[2], a2a_r.at[2], at(ry=right))
    send(wv.at[pl.ds(mult(left, q), q)], wq.at[y], a2a_s.at[3], a2a_r.at[3], at(ry=left))

    place = lax.broadcasted_iota(jnp.int32, (width, width), 0)
    column = lax.broadcasted_iota(jnp.int32, (width, width), 1)
    bits = own.bit_length() - 1
    origin = (place & (own - 1)) * nr + (place >> bits)
    pick = jnp.where(column == origin, 1.0, 0.0).astype(HALF)
    loads["c"].wait()
    cp[...] = dot_nt(pick, cv[:, pl.ds(mult(y, width), width)]).astype(HALF)
    sets = [chain_refs[9 * n : 9 * n + 9] for n in range(len(STRIDES))]
    sets[0][0][...] = dot_nt(cp[...], hid[...]) * factor

    specs = [chains_of(nr, stride) for stride in STRIDES]
    clock = [0] * len(specs)

    def local(mine, owner):
        return mine[pl.ds(mult(owner, own), own), :]

    def tick(s):
        with jax.named_scope(f"tick#s={s}"):
            step(s)

    def side_span(s, piece):
        count, size = side_count(nr, STRIDES[s]), PIECE[s]
        return range(count - size * (piece + 1), count - size * piece)

    def sides(s, c, piece):
        _, _, _, side_src, side_dst, _, _, side_s, side_r = sets[s]
        span = pl.ds(side_span(s, piece).start, PIECE[s])
        for r in range(1, STRIDES[s]):
            yield r, side_src.at[c, r - 1, span], side_dst.at[c, r - 1, span], side_s.at[c, r - 1, piece], side_r.at[c, r - 1, piece]

    def launch_sides(s, piece):
        mine, _, _, side_src, _, _, _, _, _ = sets[s]
        stride = STRIDES[s]
        for c, (way, _, _, _) in enumerate(specs[s]):
            for r in range(1, stride):
                for m in side_span(s, piece):
                    side_src[c, r - 1, m] = local(mine, rep(way * (stride * m + r))).astype(HALF)
        for c, (way, _, _, _) in enumerate(specs[s]):
            for r, src, dst, ssem, rsem in sides(s, c, piece):
                send(src, dst, ssem, rsem, at(rz=rep(way * r)))

    def launch_due(s, tau):
        if STRIDES[s] > 1:
            for piece in range(side_count(nr, STRIDES[s]) // PIECE[s]):
                if tau == max(0, 1 + PIECE[s] * piece - LEAD[s]):
                    launch_sides(s, piece)

    def step(s):
        tau = clock[s]
        clock[s] += 1
        mine, stage, buf, _, side_dst, ssem, rsem, _, _ = sets[s]
        stride = STRIDES[s]
        count, size = side_count(nr, stride), PIECE[s]
        if tau > 0:
            launch_due(s, tau)
        for c, (way, far, links, delay) in enumerate(specs[s]):
            k = tau - delay
            m = links - k
            if stride > 1 and tau % size == 1 % size and 1 <= tau <= count:
                for _, _, dst, _, rsem_side in sides(s, c, (tau - 1) // size):
                    arrived(dst, rsem_side)
            if not 0 <= k <= links:
                continue
            if k > 0:
                arrived(buf.at[c, k - 1], rsem.at[c, k - 1])
            if k == links:
                continue
            total = local(mine, rep(way * stride * m))
            for r in range(1, stride):
                if stride * m + r <= far:
                    total = total + side_dst[c, r - 1, m].astype(SINGLE)
            if k == 0:
                src = stage.at[c]
            else:
                src = buf.at[c, k - 1]
                total = total + src[...].astype(SINGLE)
            src[...] = total.astype(HALF)
            send(src, buf.at[c, k], ssem.at[c, k], rsem.at[c, k], at(rz=rep(way * stride)))
        if tau == 0:
            launch_due(s, tau)

    def length(s):
        return max(links + delay for _, _, links, delay in specs[s])

    def total_of(s):
        mine, _, buf, _, side_dst, _, _, _, _ = sets[s]
        total = local(mine, z)
        for c, (_, _, links, _) in enumerate(specs[s]):
            total = total + buf[c, links - 1].astype(SINGLE)
            for r in range(1, STRIDES[s]):
                total = total + side_dst[c, r - 1, 0].astype(SINGLE)
        return total

    tick(0)

    loads["x"].wait()
    xp[...] = dot_nt(pick, xv[...]).astype(HALF)

    arrived(relay_a, a2a_r.at[0])
    send(relay_a, wq.at[left, pl.ds(0, top)], a2a_s.at[4], a2a_r.at[4], at(ry=right))
    arrived(relay_b, a2a_r.at[1])
    send(relay_b, wq.at[right, pl.ds(top, low)], a2a_s.at[5], a2a_r.at[5], at(ry=left))
    tick(0)

    def piece(j):
        return dot_nt(wq[j], cv[:, pl.ds(mult(j, width), width)])

    loads["wq"].wait()
    arrived(wq.at[left], a2a_r.at[2])
    arrived(wq.at[right], a2a_r.at[3])
    part = piece(y) + piece(left) + piece(right)
    arrived(wq.at[across, pl.ds(0, top)], a2a_r.at[4])
    arrived(wq.at[across, pl.ds(top, low)], a2a_r.at[5])
    hgb[y] = (part + piece(across)).astype(HALF)
    upper_rows, lower_rows = pl.ds(0, top), pl.ds(top, low)
    send(hgb.at[y, upper_rows], hgb.at[y, upper_rows], hg_s.at[0], hg_r.at[0], at(ry=right))
    send(hgb.at[y, lower_rows], hgb.at[y, lower_rows], hg_s.at[1], hg_r.at[1], at(ry=left))
    send(hgb.at[y, lower_rows], hgb.at[y, lower_rows], hg_s.at[2], hg_r.at[2], at(ry=right))
    send(hgb.at[y, upper_rows], hgb.at[y, upper_rows], hg_s.at[3], hg_r.at[3], at(ry=left))

    def quarter(i):
        j = order[i]
        span = pl.ds(mult(j, q), q)
        grad = hgb[j].astype(SINGLE)
        dall[i, 0:q, :] = (grad * cg[span, :]).astype(HALF)
        dall[i, q : 2 * q, :] = (grad * cu[span, :]).astype(HALF)
        sets[1 + i][0][...] = dot_nt(xp[...], dall[i]) * factor
        tick(1 + i)

    tick(0)
    quarter(0)
    arrived(hgb.at[left, upper_rows], hg_r.at[0])
    send(hgb.at[left, upper_rows], hgb.at[left, upper_rows], hg_s.at[4], hg_r.at[4], at(ry=right))
    arrived(hgb.at[right, lower_rows], hg_r.at[1])
    send(hgb.at[right, lower_rows], hgb.at[right, lower_rows], hg_s.at[5], hg_r.at[5], at(ry=left))
    tick(0)
    tick(1)
    arrived(hgb.at[left, lower_rows], hg_r.at[2])
    quarter(1)
    arrived(hgb.at[right, upper_rows], hg_r.at[3])
    quarter(2)
    arrived(hgb.at[across, upper_rows], hg_r.at[4])
    arrived(hgb.at[across, lower_rows], hg_r.at[5])
    quarter(3)
    tick(0)

    for name in [f"w{kind}{j}" for kind in "gu" for j in range(nf)]:
        loads[name].wait()

    block = 128

    def terms(n):
        span = pl.ds(n * block, block)
        total = dot_tn(dall[0, :, span], wcat[order[0]])
        for i in range(1, nf):
            total = total + dot_tn(dall[i, :, span], wcat[order[i]])
        term[span, :] = total.astype(HALF)

    peers = [lax.rem(t + step, nt) for step in range(1, nt)]

    def terms_out():
        for n, peer in enumerate(peers):
            send(term.at[pl.ds(mult(peer, rows), rows)], parts.at[t], ti_s.at[n], ti_r.at[n], at(rt=peer))
        parts[t] = term[pl.ds(mult(t, rows), rows), :]

    def sources():
        return [lax.rem(t + nt - step, nt) for step in range(1, nt)]

    def terms_sum():
        for n, peer in enumerate(sources()):
            arrived(parts.at[peer], ti_r.at[n])
        total = parts[0].astype(SINGLE)
        for n in range(1, nt):
            total = total + parts[n].astype(SINGLE)
        res[...] = total.astype(HALF)
        for n, peer in enumerate(peers):
            send(res, gi_ref.at[t], to_s.at[n], to_r.at[n], at(rt=peer))
        pltpu.make_async_copy(res, gi_ref.at[t], out_sem).start()

    def terms_end():
        for n, peer in enumerate(sources()):
            arrived(gi_ref.at[peer], to_r.at[n])
        pltpu.make_async_copy(res, gi_ref.at[t], out_sem).wait()

    group = 4
    inner, outer = lax.rem(z, group), z // group
    count = nr // group

    def down_first():
        total = total_of(0)
        gd_ref[...] = total
        dnear[inner, y] = jnp.sum(total * total, axis=0, keepdims=True)
        for n in range(1, group * nf):
            by_z, by_y = n // nf, n % nf
            device = at(rz=outer * group + lax.rem(inner + by_z, group), ry=lax.rem(y + by_y, nf))
            send(dnear.at[inner, y], dnear.at[inner, y], m_s.at[n - 1], m_r.at[n - 1], device)

    def down_second():
        for n in range(1, group * nf):
            by_z, by_y = n // nf, n % nf
            place = dnear.at[lax.rem(inner + group - by_z, group), lax.rem(y + nf - by_y, nf)]
            arrived(place, m_r.at[n - 1])
        total = dnear[0, 0]
        for n in range(1, group * nf):
            total = total + dnear[n // nf, n % nf]
        dfar[outer] = total
        for n in range(1, count):
            device = at(rz=lax.rem(outer + n, count) * group + inner)
            send(dfar.at[outer], dfar.at[outer], f_s.at[n - 1], f_r.at[n - 1], device)

    def down_last():
        for n in range(1, count):
            arrived(dfar.at[lax.rem(outer + count - n, count)], f_r.at[n - 1])
        total = dfar[0]
        for n in range(1, count):
            total = total + dfar[n]
        dn_ref[...] = total

    blocks = tokens // block
    input_stage = [functools.partial(terms, n) for n in range(blocks)]
    input_stage += [terms_out] + [lambda: None] * WAITS + [terms_sum]
    down_stage = [down_first, down_second]
    n_tick = 0
    while any(clock[s] <= length(s) for s in ROUND):
        n_tick += 1
        for s in ROUND:
            if clock[s] <= length(s):
                tick(s)
        for _ in range(PER_TICK):
            if input_stage:
                input_stage.pop(0)()
        if clock[0] > length(0) and down_stage:
            down_stage.pop(0)()
    for stage in input_stage + down_stage:
        stage()

    for i in range(nf):
        fin[order[i]] = total_of(1 + i)
    gate_total = jnp.zeros((own, 1), SINGLE)
    up_total = jnp.zeros((own, 1), SINGLE)
    for j in range(nf):
        gate_part, up_part = fin[j, :, 0:q], fin[j, :, q : 2 * q]
        gg_ref[:, j * q : (j + 1) * q] = gate_part
        gu_ref[:, j * q : (j + 1) * q] = up_part
        gate_total = gate_total + jnp.sum(gate_part * gate_part, axis=1, keepdims=True)
        up_total = up_total + jnp.sum(up_part * up_part, axis=1, keepdims=True)
    lane = lax.broadcasted_iota(jnp.int32, (own, 128), 1)
    nvec[...] = jnp.where(lane < 64, gate_total, up_total)
    nrecv[t] = nvec[...]
    for n, peer in enumerate(peers):
        send(nvec, nrecv.at[t], n_s.at[n], n_r.at[n], at(rt=peer))
    terms_end()
    for n, peer in enumerate(sources()):
        arrived(nrecv.at[peer], n_r.at[n])
    norms = nrecv[0]
    for n in range(1, nt):
        norms = norms + nrecv[n]
    turned = norms.T
    gn_ref[...] = turned[0:1, :]
    un_ref[...] = turned[64:65, :]
    down_last()
    for copy in sent:
        copy.wait_send()


def finish(gi_ref, gg_ref, gu_ref, gd_ref, gn_ref, un_ref, dn_ref, *out):
    gi_out, gg_out, gu_out, gd_out, gn_out, un_out, dn_out = out
    gi_out[...] = gi_ref[...]
    for src, dst in ((gg_ref, gg_out), (gu_ref, gu_out), (gd_ref, gd_out)):
        dst[...] = src[...].reshape(dst.shape)
    gn_out[...] = gn_ref[...]
    un_out[...] = un_ref[...]
    dn_out[...] = dn_ref[0, :]


def on_device(inputs, gate_pre, up_pre, cotangent, w_gate, w_up, w_down):
    nr, nf, nt = (lax.axis_size(name) for name in ("rep", "fs", "tp"))
    tokens, width = inputs.shape
    hunits = w_gate.shape[1]
    q, own, rows = hunits // nf, width // nr, tokens // nt
    top = -(-q // 32) * 16
    features = cotangent.shape[1]
    vmem, dma = pltpu.VMEM, pltpu.SemaphoreType.DMA
    any_space = pl.BlockSpec(memory_space=pl.ANY)
    in_vmem = pl.BlockSpec(memory_space=pltpu.VMEM)
    shape = jax.ShapeDtypeStruct
    chain_scratch = []
    for stride, size, lanes in zip(STRIDES, PIECE, (hunits,) + (2 * q,) * nf):
        links = nr // 2 // stride
        side = (2, max(stride - 1, 1), side_count(nr, stride))
        chain_scratch += [
            vmem((width, lanes), SINGLE),
            vmem((2, own, lanes), HALF),
            vmem((2, links, own, lanes), HALF),
            vmem((*side, own, lanes), HALF),
            vmem((*side, own, lanes), HALF),
            dma((2, links)),
            dma((2, links)),
            dma((2, side[1], side[2] // size)),
            dma((2, side[1], side[2] // size)),
        ]
    gi, gg, gu, gd, gn, un, dn = pl.pallas_call(
        functools.partial(kernel, (nr, nf, nt)),
        out_shape=(
            shape((nt, rows, width), HALF),
            shape((own, hunits), SINGLE),
            shape((own, hunits), SINGLE),
            shape((own, hunits), SINGLE),
            shape((1, own), SINGLE),
            shape((1, own), SINGLE),
            shape((1, hunits), SINGLE),
        ),
        in_specs=[any_space] * 7,
        out_specs=(any_space,) + (in_vmem,) * 6,
        scratch_shapes=[
            vmem((tokens, width), HALF),
            vmem((hunits, tokens), HALF),
            vmem((hunits, tokens), HALF),
            vmem((tokens, features), HALF),
            vmem((hunits, width), HALF),
            vmem((nf, 2 * q, width), HALF),
            vmem((nf, q, width), HALF),
            vmem((top, width), HALF),
            vmem((q - top, width), HALF),
            vmem((nf, q, tokens), HALF),
            vmem((hunits, tokens), SINGLE),
            vmem((hunits, tokens), SINGLE),
            vmem((hunits, tokens), HALF),
            vmem((width, tokens), HALF),
            vmem((width, tokens), HALF),
            vmem((nf, 2 * q, tokens), HALF),
            vmem((nf, own, 2 * q), SINGLE),
            vmem((tokens, width), HALF),
            vmem((nt, rows, width), HALF),
            vmem((rows, width), HALF),
            vmem((own, 128), SINGLE),
            vmem((nt, own, 128), SINGLE),
            vmem((4, nf, 1, hunits), SINGLE),
            vmem((nr // 4, 1, hunits), SINGLE),
            dma((6 + 2 * nf,)),
            dma((6,)),
            dma((6,)),
            dma((6,)),
            dma((6,)),
            dma((nt - 1,)),
            dma((nt - 1,)),
            dma((nt - 1,)),
            dma((nt - 1,)),
            dma((nt - 1,)),
            dma((nt - 1,)),
            dma((4 * nf - 1,)),
            dma((4 * nf - 1,)),
            dma((nr // 4 - 1,)),
            dma((nr // 4 - 1,)),
            dma(()),
            *chain_scratch,
        ],
        compiler_params=pltpu.CompilerParams(
            collective_id=0, has_side_effects=True, vmem_limit_bytes=56 * 2**20
        ),
    )(inputs, gate_pre.T, up_pre.T, cotangent, w_gate.T, w_up.T, w_down)
    gi, gg, gu, gd, gn, un, dn = pl.pallas_call(
        finish,
        out_shape=(
            shape((nt, rows, width), HALF),
            shape((own, 1, hunits), SINGLE),
            shape((own, 1, hunits), SINGLE),
            shape((own, 1, hunits), SINGLE),
            shape((1, own), SINGLE),
            shape((1, own), SINGLE),
            shape((hunits,), SINGLE),
        ),
        in_specs=[in_vmem] * 7,
        out_specs=(in_vmem,) * 7,
    )(gi, gg, gu, gd, gn, un, dn)
    return (
        gi.reshape(tokens, width),
        gg,
        gu,
        gd.transpose(2, 0, 1),
        gn.reshape(own, 1),
        un.reshape(own, 1),
        dn,
    )


def solution(mesh):
    placed = (
        P("rep", "fs"),
        P("rep", "tp"),
        P("rep", "tp"),
        P("rep", None),
        P("fs", "tp"),
        P("fs", "tp"),
        P("tp", "fs"),
    )
    return jax.shard_map(
        on_device,
        mesh=mesh,
        in_specs=placed,
        out_specs=(
            P("rep", "fs"),
            P("fs", "rep", "tp"),
            P("fs", "rep", "tp"),
            P("tp", "fs", "rep"),
            P("fs", "rep"),
            P("fs", "rep"),
            P("tp"),
        ),
        check_vma=False,
    )
```
